32 devices in a mesh: rep: 2 (over x), fs: 8 (over z, y), tp: 2 (over core).
Axes of the slice: x: 2, y: 2, z: 4, core: 2. Of those that a mesh axis runs over, the one named last changes fastest.
Arguments:
- incoming_features: bfloat16 [3072, 2048], P(('rep', 'fs'), 'tp'), may hold values from -6 to 6
- attend_prenormal_scale: bfloat16 [2048], replicated, may hold values from 0.099609375 to 1.8984375
- probe_matrix: bfloat16 [2048, 512], P('fs', 'tp'), may hold values from -0.125 to 0.125
- lookup_matrix: bfloat16 [2048, 512], P('fs', 'tp'), may hold values from -0.125 to 0.125
- content_matrix: bfloat16 [2048, 1024], P('fs', 'tp'), may hold values from -0.125 to 0.125
- forgetting_matrix: bfloat16 [2048, 512], P('fs', 'tp'), may hold values from -0.125 to 0.125
- result_switch_matrix: bfloat16 [2048, 1024], P('fs', 'tp'), may hold values from -0.125 to 0.125
- forgetting_shift: float32 [512], P('tp'), may hold values from -0.5 to 5.5
- spike_forget_logarithm: float32 [3072, 512], P(('rep', 'fs'), 'tp'), may hold values from -0.7 to 0
- attend_unit_scale: bfloat16 [1024], P('tp'), may hold values from 0.099609375 to 1.8984375
- attend_result_matrix: bfloat16 [1024, 2048], P('tp', 'fs'), may hold values from -0.1875 to 0.1875
- perceptron_scale: bfloat16 [2048], replicated, may hold values from 0.099609375 to 1.8984375
- content_expand_matrix: bfloat16 [2048, 4096], P('fs', 'tp'), may hold values from -0.125 to 0.125
- switch_expand_matrix: bfloat16 [2048, 4096], P('fs', 'tp'), may hold values from -0.125 to 0.125
- content_kernel: bfloat16 [3, 4096], P(None, 'tp'), may hold values from -3.5 to 3.5
- switch_kernel: bfloat16 [3, 4096], P(None, 'tp'), may hold values from -3.5 to 3.5
- contract_matrix: bfloat16 [4096, 2048], P('tp', 'fs'), may hold values from -0.09375 to 0.09375
Outputs:
- out_rows: bfloat16 [3072, 2048], P(('rep', 'fs'), 'tp')
The draws below stay inside these ranges and needn't reach their ends.
All inputs are finite; a program needn't handle non-finite values.
Results may differ from the reference program's by a relative error of at most 0.02.
Values may be sent and summed in bfloat16 or wider, within the bound.
A program may use at most 64 MiB of HBM per device.

```python
import math
import jax
import jax.numpy as jnp
from jax import lax

EMBED_DIM = 2048
HEAD_K = 32
HEAD_V = 64
FF = 4096
BLOCK = 64
CONTEXT_SPAN = 192
LOOKUP_FEATURES = 512
VAL_W = 1024
BATCH_SIZE = 16
TOKENS = 3072
N_TP = 2


def draw_forgetting_shift(key, part):
    head_count = LOOKUP_FEATURES // HEAD_K
    key_slow, key_high, key_low = jax.random.split(jax.random.fold_in(key, 11), 3)
    slow = jax.random.uniform(key_slow, (head_count,)) < 0.5
    slow_channels = jnp.repeat(slow, HEAD_K)
    high = jax.random.uniform(key_high, (LOOKUP_FEATURES,), jnp.float32, 3.5, 5.5)
    low = jax.random.uniform(key_low, (LOOKUP_FEATURES,), jnp.float32, -0.5, 1.0)
    return jnp.where(slow_channels, high, low).astype(jnp.float32)


def draw_spike_forget_logarithm(key, part):
    head_count = LOOKUP_FEATURES // HEAD_K
    key_hit, key_depth = jax.random.split(jax.random.fold_in(key, 23))
    hits = jax.random.uniform(key_hit, (TOKENS, head_count)) < 6.0 / CONTEXT_SPAN
    depth = jax.random.uniform(key_depth, (TOKENS, head_count), jnp.float32, math.log(0.5), math.log(0.8))
    return jnp.repeat(jnp.where(hits, depth, 0.0), HEAD_K, axis=1).astype(jnp.float32)


def level_of(own_key, shape, pieces, smallest, top_value):
    factor_of, own = 1.0, jax.random.fold_in(own_key, 6)
    for position, parts in pieces:
        steps = jnp.exp(jax.random.uniform(jax.random.fold_in(own, position), (parts,), jnp.float32, smallest / len(pieces), top_value / len(pieces)))
        factor_of = factor_of * jnp.repeat(steps, shape[position] // parts).reshape([-1 if axis == position else 1 for axis in range(len(shape))])
    return factor_of


def gaussian(own_key, dims, spread, limit, cuts=(), held_as=jnp.bfloat16):
    factor_of = level_of(own_key, dims, cuts, -0.22, 0.18) if cuts else 1.0
    values = jax.random.normal(own_key, dims, jnp.float32) * spread * factor_of
    return jnp.minimum(jnp.maximum(values, -limit), limit).astype(held_as)


def setup_inputs(seed: int = 0) -> dict:
    streams_of = jax.random.split(jax.random.key(seed), 18)
    incoming_features = gaussian(streams_of[0], (TOKENS, EMBED_DIM), 1.0, 6.0, ((0, 16), (1, 2)))
    attend_prenormal_scale = jnp.clip(1.0 + 0.18 * jax.random.normal(streams_of[1], (EMBED_DIM,), jnp.float32), 0.099609375, 1.8984375).astype(jnp.bfloat16)
    probe_matrix = gaussian(streams_of[2], (EMBED_DIM, LOOKUP_FEATURES), EMBED_DIM ** -0.5, 0.125, ((0, 8), (1, 2)))
    lookup_matrix = gaussian(streams_of[3], (EMBED_DIM, LOOKUP_FEATURES), EMBED_DIM ** -0.5, 0.125, ((0, 8), (1, 2)))
    content_matrix = gaussian(streams_of[4], (EMBED_DIM, VAL_W), EMBED_DIM ** -0.5, 0.125, ((0, 8), (1, 2)))
    forgetting_matrix = gaussian(streams_of[5], (EMBED_DIM, LOOKUP_FEATURES), EMBED_DIM ** -0.5, 0.125, ((0, 8), (1, 2)))
    result_switch_matrix = gaussian(streams_of[6], (EMBED_DIM, VAL_W), EMBED_DIM ** -0.5, 0.125, ((0, 8), (1, 2)))
    forgetting_shift = draw_forgetting_shift(jax.random.fold_in(streams_of[17], 71), 0)
    spike_forget_logarithm = draw_spike_forget_logarithm(jax.random.fold_in(streams_of[17], 71), 0)
    attend_unit_scale = jnp.clip(1.0 + 0.18 * jax.random.normal(streams_of[9], (VAL_W,), jnp.float32), 0.099609375, 1.8984375).astype(jnp.bfloat16)
    attend_result_matrix = gaussian(streams_of[10], (VAL_W, EMBED_DIM), VAL_W ** -0.5, 0.1875, ((0, 2), (1, 8)))
    perceptron_scale = jnp.clip(1.0 + 0.18 * jax.random.normal(streams_of[11], (EMBED_DIM,), jnp.float32), 0.099609375, 1.8984375).astype(jnp.bfloat16)
    content_expand_matrix = gaussian(streams_of[12], (EMBED_DIM, FF), EMBED_DIM ** -0.5, 0.125, ((0, 8), (1, 2)))
    switch_expand_matrix = gaussian(streams_of[13], (EMBED_DIM, FF), EMBED_DIM ** -0.5, 0.125, ((0, 8), (1, 2)))
    content_kernel = gaussian(streams_of[14], (3, FF), 3 ** -0.5, 3.5, ((1, 2),))
    switch_kernel = gaussian(streams_of[15], (3, FF), 3 ** -0.5, 3.5, ((1, 2),))
    contract_matrix = gaussian(streams_of[16], (FF, EMBED_DIM), FF ** -0.5, 0.09375, ((0, 2), (1, 8)))
    return {"incoming_features": incoming_features, "attend_prenormal_scale": attend_prenormal_scale, "probe_matrix": probe_matrix, "lookup_matrix": lookup_matrix, "content_matrix": content_matrix, "forgetting_matrix": forgetting_matrix, "result_switch_matrix": result_switch_matrix, "forgetting_shift": forgetting_shift, "spike_forget_logarithm": spike_forget_logarithm, "attend_unit_scale": attend_unit_scale, "attend_result_matrix": attend_result_matrix, "perceptron_scale": perceptron_scale, "content_expand_matrix": content_expand_matrix, "switch_expand_matrix": switch_expand_matrix, "content_kernel": content_kernel, "switch_kernel": switch_kernel, "contract_matrix": contract_matrix}


norm_eps = 1e-06
switch_multiplier = 16.0

def row_norm(content_tokens, gain):
    content_tokens = content_tokens.astype(jnp.float32)
    scaled = content_tokens * lax.rsqrt(lax.optimization_barrier(jnp.mean(content_tokens * content_tokens, axis=-1, keepdims=True)) + norm_eps)
    return (scaled * gain.astype(jnp.float32)).astype(jnp.bfloat16)

def gated_scan(probe_tokens, lookup_tokens, content_tokens, forgetting_scores):
    length, heads, key_size = probe_tokens.shape
    value_size = content_tokens.shape[-1]
    blocks = length // BLOCK

    def split_blocks(array):
        return array.reshape(blocks, BLOCK, heads, array.shape[-1])
    causal = jnp.arange(BLOCK)[:, None] >= jnp.arange(BLOCK)[None, :]
    highest = lax.Precision.HIGHEST

    def step(state, incoming_tokens):
        query_block, key_block, value_block, decay_block = incoming_tokens
        cumulative = jnp.cumsum(decay_block, axis=0)
        differ = cumulative[:, None] - cumulative[None, :]
        weight = jnp.exp(jnp.where(causal[:, :, None, None], differ, -jnp.inf))
        scores = jnp.einsum('thd,shd,tshd->tsh', query_block, key_block, weight, precision=highest)
        inner = jnp.einsum('tsh,shv->thv', scores, value_block, precision=highest)
        carried = jnp.einsum('thd,hdv->thv', query_block * jnp.exp(cumulative), state, precision=highest)
        final = cumulative[-1]
        state = jnp.exp(final)[:, :, None] * state + jnp.einsum('shd,shv->hdv', key_block * jnp.exp(final[None] - cumulative), value_block, precision=highest)
        return (state, inner + carried)
    start_state = jnp.zeros((heads, key_size, value_size), jnp.float32)
    _, result_tokens = lax.scan(step, start_state, (split_blocks(probe_tokens), split_blocks(lookup_tokens), split_blocks(content_tokens), split_blocks(forgetting_scores)))
    return result_tokens.reshape(length, heads, value_size)

def attend_unit_results(probe_tokens, lookup_tokens, content_tokens, result_switch, forgetting_raw, spike_forgetting, attend_unit_scale):
    length = probe_tokens.shape[0]
    heads = probe_tokens.shape[1] // HEAD_K
    forgetting_scores = jax.nn.log_sigmoid(forgetting_raw) / switch_multiplier + spike_forgetting

    def split_heads(array, width):
        return array.astype(jnp.float32).reshape(length, heads, width)
    result_tokens = gated_scan(split_heads(probe_tokens, HEAD_K) * HEAD_K ** (-0.5), split_heads(lookup_tokens, HEAD_K), split_heads(content_tokens, HEAD_V), split_heads(forgetting_scores, HEAD_K))
    result_tokens = result_tokens * lax.rsqrt(lax.optimization_barrier(jnp.mean(result_tokens * result_tokens, axis=-1, keepdims=True)) + norm_eps)
    result_tokens = result_tokens * attend_unit_scale.astype(jnp.float32).reshape(heads, HEAD_V)
    switched_result = result_tokens.reshape(length, heads * HEAD_V) * jax.nn.silu(result_switch.astype(jnp.float32))
    return switched_result.astype(jnp.bfloat16)

def causal_conv(content_tokens, taps):
    content_tokens = content_tokens.astype(jnp.float32)
    taps = taps.astype(jnp.float32)
    width = taps.shape[0]
    padded = jnp.pad(content_tokens, ((width - 1, 0), (0, 0)))
    total = jnp.zeros_like(content_tokens)
    for offset in range(width):
        total = total + padded[offset:offset + content_tokens.shape[0]] * taps[offset]
    return total

def grouped_product(content_tokens, weight):
    group = content_tokens.shape[1] // N_TP
    total = jnp.zeros((content_tokens.shape[0], weight.shape[1]), jnp.float32)
    for index in range(N_TP):
        partial_sum = jnp.dot(content_tokens[:, index * group:(index + 1) * group], weight[index * group:(index + 1) * group], preferred_element_type=jnp.float32)
        total = total + lax.optimization_barrier(partial_sum.astype(jnp.bfloat16)).astype(jnp.float32)
    return total.astype(jnp.bfloat16)

def reference(incoming_features, attend_prenormal_scale, probe_matrix, lookup_matrix, content_matrix, forgetting_matrix, result_switch_matrix, forgetting_shift, spike_forget_logarithm, attend_unit_scale, attend_result_matrix, perceptron_scale, content_expand_matrix, switch_expand_matrix, content_kernel, switch_kernel, contract_matrix):

    def lone_context(incoming_tokens):
        weight_fragments, spike_forgetting = incoming_tokens
        normed = row_norm(weight_fragments, attend_prenormal_scale)
        probe_tokens = jnp.dot(normed, probe_matrix, preferred_element_type=jnp.float32).astype(jnp.bfloat16)
        lookup_tokens = jnp.dot(normed, lookup_matrix, preferred_element_type=jnp.float32).astype(jnp.bfloat16)
        content_tokens = jnp.dot(normed, content_matrix, preferred_element_type=jnp.float32).astype(jnp.bfloat16)
        result_switch = jnp.dot(normed, result_switch_matrix, preferred_element_type=jnp.float32).astype(jnp.bfloat16)
        forgetting_raw = jnp.dot(normed, forgetting_matrix, preferred_element_type=jnp.float32) + forgetting_shift
        switched_result = attend_unit_results(probe_tokens, lookup_tokens, content_tokens, result_switch, forgetting_raw, spike_forgetting, attend_unit_scale)
        mix = grouped_product(switched_result, attend_result_matrix)
        middle = (weight_fragments.astype(jnp.float32) + lax.optimization_barrier(mix).astype(jnp.float32)).astype(jnp.bfloat16)
        normed_mid = row_norm(middle, perceptron_scale)
        up_value = jnp.dot(normed_mid, content_expand_matrix, preferred_element_type=jnp.float32).astype(jnp.bfloat16)
        up_gate = jnp.dot(normed_mid, switch_expand_matrix, preferred_element_type=jnp.float32).astype(jnp.bfloat16)
        conv_value = causal_conv(up_value, content_kernel)
        conv_gated = causal_conv(up_gate, switch_kernel)
        hidden = (conv_value * jax.nn.gelu(conv_gated, approximate=True)).astype(jnp.bfloat16)
        ffn = grouped_product(hidden, contract_matrix)
        return (middle.astype(jnp.float32) + lax.optimization_barrier(ffn).astype(jnp.float32)).astype(jnp.bfloat16)
    result_tokens = lax.map(lone_context, (incoming_features.reshape(BATCH_SIZE, CONTEXT_SPAN, EMBED_DIM), spike_forget_logarithm.reshape(BATCH_SIZE, CONTEXT_SPAN, LOOKUP_FEATURES)))
    return result_tokens.reshape(TOKENS, EMBED_DIM)
```

```python
import functools

import jax
import jax.numpy as jnp
from jax import lax
from jax.experimental import pallas as pl
from jax.experimental.pallas import tpu as pltpu
from jax.sharding import PartitionSpec as P

HEAD_K = 32
HEAD_V = 64
SUB = 16

norm_eps = 1e-06
switch_multiplier = 16.0
MESH = pl.DeviceIdType.MESH
F32 = jnp.float32
BF16 = jnp.bfloat16
HIGHEST = lax.Precision.HIGHEST
VMEM_LIMIT = 60 * 1024 * 1024


def row_norm(content_tokens, gain):
    content_tokens = content_tokens.astype(F32)
    scaled = content_tokens * lax.rsqrt(
        jnp.mean(content_tokens * content_tokens, axis=-1, keepdims=True) + norm_eps
    )
    return (scaled * gain.astype(F32)).astype(BF16)


def factor(n):
    inner = 1
    for size in range(1, n + 1):
        if n % size == 0 and size * size <= n:
            inner = size
    return n // inner, inner


def place(ref, axis, index, size):
    at = pl.ds(pl.multiple_of(index * size, size), size)
    return ref.at[at, :] if axis == 0 else ref.at[:, at]


def gather_weights(pieces, axes, group_piece, sizes, collective_id):
    n_rep, n_fs, n_tp = sizes
    outer, inner = factor(n_fs)
    count = len(pieces)
    has_group = group_piece is not None
    group = n_rep * n_tp
    full = []
    for piece, axis in zip(pieces, axes):
        shape = list(piece.shape)
        shape[axis] *= n_fs
        full.append(jax.ShapeDtypeStruct(tuple(shape), piece.dtype))
    ins = list(pieces)
    if has_group:
        ins.append(group_piece)
        full.append(
            jax.ShapeDtypeStruct(
                (group_piece.shape[0] * n_rep, group_piece.shape[1] * n_tp), group_piece.dtype
            )
        )

    def kernel(*refs):
        sources = refs[: len(ins)]
        outs = refs[len(ins) : 2 * len(ins)]
        far_send, far_recv, near_send, near_recv, own_sem, group_send, group_recv = refs[
            2 * len(ins) :
        ]
        rep, fs, tp = lax.axis_index("rep"), lax.axis_index("fs"), lax.axis_index("tp")
        a, b = fs // inner, lax.rem(fs, inner)
        far = [lax.rem(a + d, outer) * inner + b for d in range(1, outer)]
        near = [a * inner + lax.rem(b + d, inner) for d in range(1, inner)]
        barrier = pltpu.get_barrier_semaphore()
        peers = [{"fs": index} for index in far + near]
        others = []
        if has_group:
            for i in range(n_rep):
                for j in range(n_tp):
                    if i or j:
                        others.append(
                            {"rep": lax.rem(rep + i, n_rep), "tp": lax.rem(tp + j, n_tp)}
                        )
        for peer in peers + others:
            pl.semaphore_signal(barrier, inc=1, device_id=peer, device_id_type=MESH)
        pl.semaphore_wait(barrier, len(peers) + len(others))

        waits = []
        if has_group:
            rows, columns = group_piece.shape
            source, out = sources[-1], outs[-1]
            target = out.at[
                pl.ds(pl.multiple_of(rep * rows, rows), rows),
                pl.ds(pl.multiple_of(tp * columns, columns), columns),
            ]
            own = pltpu.make_async_copy(source, target, own_sem.at[count])
            own.start()
            waits.append(own)
            for d, peer in enumerate(others):
                copy = pltpu.make_async_remote_copy(
                    src_ref=source,
                    dst_ref=target,
                    send_sem=group_send.at[d],
                    recv_sem=group_recv.at[d],
                    device_id=peer,
                    device_id_type=MESH,
                )
                copy.start()
                waits.append(copy)
        far_copies = []
        for w in range(count):
            axis, size = axes[w], pieces[w].shape[axes[w]]
            target = place(outs[w], axis, fs, size)
            copies = []
            for d, index in enumerate(far):
                copy = pltpu.make_async_remote_copy(
                    src_ref=sources[w],
                    dst_ref=target,
                    send_sem=far_send.at[w, d],
                    recv_sem=far_recv.at[w, d],
                    device_id={"fs": index},
                    device_id_type=MESH,
                )
                copy.start()
                copies.append(copy)
            far_copies.append(copies)
            for e, index in enumerate(near):
                copy = pltpu.make_async_remote_copy(
                    src_ref=sources[w],
                    dst_ref=target,
                    send_sem=near_send.at[w, 0, e],
                    recv_sem=near_recv.at[w, 0, e],
                    device_id={"fs": index},
                    device_id_type=MESH,
                )
                copy.start()
                waits.append(copy)
            own = pltpu.make_async_copy(sources[w], target, own_sem.at[w])
            own.start()
            waits.append(own)
        for w in range(count):
            axis, size = axes[w], pieces[w].shape[axes[w]]
            for d in range(1, outer):
                far_copies[w][d - 1].wait_recv()
                block = place(outs[w], axis, lax.rem(a + outer - d, outer) * inner + b, size)
                for e, index in enumerate(near):
                    copy = pltpu.make_async_remote_copy(
                        src_ref=block,
                        dst_ref=block,
                        send_sem=near_send.at[w, d, e],
                        recv_sem=near_recv.at[w, d, e],
                        device_id={"fs": index},
                        device_id_type=MESH,
                    )
                    copy.start()
                    waits.append(copy)
        for copies in far_copies:
            for copy in copies:
                copy.wait_send()
        for copy in waits:
            copy.wait()

    dma = pltpu.SemaphoreType.DMA
    return pl.pallas_call(
        kernel,
        out_shape=full,
        in_specs=[pl.BlockSpec(memory_space=pltpu.VMEM)] * len(ins),
        out_specs=[pl.BlockSpec(memory_space=pl.ANY)] * len(ins),
        scratch_shapes=[
            dma((count, max(outer - 1, 1))),
            dma((count, max(outer - 1, 1))),
            dma((count, outer, max(inner - 1, 1))),
            dma((count, outer, max(inner - 1, 1))),
            dma((count + 1,)),
            dma((group,)),
            dma((group,)),
        ],
        compiler_params=pltpu.CompilerParams(
            collective_id=collective_id, has_side_effects=True, vmem_limit_bytes=VMEM_LIMIT
        ),
        name="gather_weights",
    )(*ins)


def reduce_group(partial, base, sizes, spread, collective_id):
    n_rep, n_fs, n_tp = sizes
    rows, columns = base.shape

    def kernel(*refs):
        part_ref, base_ref = refs[:2]
        if spread:
            out_ref, all_ref, slot_a, held, slot_b, send_sem, recv_sem = refs[2:]
        else:
            out_ref, slot_a, held, slot_b, send_sem, recv_sem = refs[2:]
        rep, tp = lax.axis_index("rep"), lax.axis_index("tp")
        tps = [lax.rem(tp + d, n_tp) for d in range(1, n_tp)]
        reps = [lax.rem(rep + d, n_rep) for d in range(1, n_rep)]
        barrier = pltpu.get_barrier_semaphore()
        for index in tps:
            pl.semaphore_signal(barrier, inc=1, device_id={"tp": index}, device_id_type=MESH)
        for index in reps:
            pl.semaphore_signal(barrier, inc=1, device_id={"rep": index}, device_id_type=MESH)
        pl.semaphore_wait(barrier, len(tps) + len(reps))

        def send(stage, d, source, target, peer):
            copy = pltpu.make_async_remote_copy(
                src_ref=source,
                dst_ref=target,
                send_sem=send_sem.at[stage, d],
                recv_sem=recv_sem.at[stage, d],
                device_id=peer,
                device_id_type=MESH,
            )
            copy.start()
            return copy

        copies = [
            send(0, d, place(part_ref, 1, index, columns), slot_a.at[d], {"tp": index})
            for d, index in enumerate(tps)
        ]
        for copy in copies:
            copy.wait()
        total = place(part_ref, 1, tp, columns)[...].astype(F32)
        for d in range(len(tps)):
            total = total + slot_a[d].astype(F32)
        held[...] = total.astype(BF16)
        copies = [
            send(1, d, place(held, 0, index, rows), slot_b.at[d], {"rep": index})
            for d, index in enumerate(reps)
        ]
        for copy in copies:
            copy.wait()
        total = place(held, 0, rep, rows)[...].astype(F32)
        for d in range(len(reps)):
            total = total + slot_b[d].astype(F32)
        result = (base_ref[...].astype(F32) + total.astype(BF16).astype(F32)).astype(BF16)
        out_ref[...] = result
        if spread:
            block = all_ref.at[
                pl.ds(pl.multiple_of(rep * rows, rows), rows),
                pl.ds(pl.multiple_of(tp * columns, columns), columns),
            ]
            block[...] = result
            copies = [send(2, d, block, block, {"rep": index}) for d, index in enumerate(reps)]
            for copy in copies:
                copy.wait()
            strip = place(all_ref, 1, tp, columns)
            copies = [send(3, d, strip, strip, {"tp": index}) for d, index in enumerate(tps)]
            for copy in copies:
                copy.wait()

    out_shape = [jax.ShapeDtypeStruct((rows, columns), BF16)]
    if spread:
        out_shape.append(jax.ShapeDtypeStruct((rows * n_rep, columns * n_tp), BF16))
    vmem = pl.BlockSpec(memory_space=pltpu.VMEM)
    most = max(n_rep, n_tp)
    return pl.pallas_call(
        kernel,
        out_shape=out_shape,
        in_specs=[vmem, vmem],
        out_specs=[vmem] * len(out_shape),
        scratch_shapes=[
            pltpu.VMEM((max(n_tp - 1, 1), rows * n_rep, columns), BF16),
            pltpu.VMEM((rows * n_rep, columns), BF16),
            pltpu.VMEM((max(n_rep - 1, 1), rows, columns), BF16),
            pltpu.SemaphoreType.DMA((4, most)),
            pltpu.SemaphoreType.DMA((4, most)),
        ],
        compiler_params=pltpu.CompilerParams(
            collective_id=collective_id, has_side_effects=True, vmem_limit_bytes=VMEM_LIMIT
        ),
        name="reduce_group",
    )(partial, base)


def lanes_same(shape, row_width, column_width):
    return (
        lax.broadcasted_iota(jnp.int32, shape, 0) // row_width
        == lax.broadcasted_iota(jnp.int32, shape, 1) // column_width
    ).astype(F32)


def dot32(left, right, contract=((1,), (0,))):
    return lax.dot_general(
        left, right, (contract, ((), ())), precision=HIGHEST, preferred_element_type=F32
    )


def attend_kernel(sums_ref, shift_ref, spike_ref, scale_ref, out_ref, *, heads):
    length = sums_ref.shape[0]
    key_lanes, value_lanes = heads * HEAD_K, heads * HEAD_V

    def part(start, width):
        return sums_ref[:, start : start + width]

    def rounded(array):
        return array.astype(BF16).astype(F32)

    query = rounded(part(0, key_lanes)) * HEAD_K ** (-0.5)
    keys = rounded(part(key_lanes, key_lanes))
    values = rounded(part(2 * key_lanes, value_lanes))
    decay_pre = part(2 * key_lanes + value_lanes, key_lanes) + shift_ref[...]
    gate = rounded(part(3 * key_lanes + value_lanes, value_lanes))
    log_sigmoid = jnp.minimum(decay_pre, 0.0) - jnp.log1p(jnp.exp(-jnp.abs(decay_pre)))
    c = log_sigmoid / switch_multiplier + spike_ref[...]
    row = lax.broadcasted_iota(jnp.int32, (length, key_lanes), 0)
    step = 1
    while step < length:
        c = c + jnp.where(row >= step, pltpu.roll(c, step, 0), 0.0)
        step *= 2

    spread = lanes_same((key_lanes, value_lanes), HEAD_K, HEAD_V)
    in_sub = lax.rem(row, SUB)
    out = dot32(query * keys, spread) * values
    for d in range(1, SUB):
        ok = in_sub >= d
        weight = jnp.exp(jnp.where(ok, c - pltpu.roll(c, d, 0), 0.0))
        product = jnp.where(ok, query * pltpu.roll(keys, d, 0) * weight, 0.0)
        out = out + dot32(product, spread) * pltpu.roll(values, d, 0)

    pieces = [jnp.zeros((SUB, value_lanes), F32)]
    stack = heads * SUB
    key_mask = lanes_same((stack, key_lanes), SUB, HEAD_K)
    value_mask = lanes_same((stack, value_lanes), SUB, HEAD_V)
    for start in range(SUB, length, SUB):
        edge = c[start - 1 : start]
        q_part = query[start : start + SUB] * jnp.exp(c[start : start + SUB] - edge)
        k_part = keys[:start] * jnp.exp(edge - c[:start])
        stacked = jnp.concatenate([q_part] * heads, axis=0) * key_mask
        scores = dot32(stacked, k_part, ((1,), (1,)))
        read = dot32(scores, values[:start]) * value_mask
        total = read[:SUB]
        for h in range(1, heads):
            total = total + read[h * SUB : (h + 1) * SUB]
        pieces.append(total)
    out = out + jnp.concatenate(pieces, axis=0)

    same = lanes_same((value_lanes, value_lanes), HEAD_V, HEAD_V)
    mean = dot32(out * out, same) / HEAD_V
    out = out * lax.rsqrt(mean + norm_eps) * scale_ref[...]
    out_ref[...] = (out * (gate / (1.0 + jnp.exp(-gate)))).astype(BF16)


def attend(sums, shift, spike, scale, length):
    heads = shift.shape[0] // HEAD_K
    value_lanes = heads * HEAD_V
    rows = sums.shape[0]
    return pl.pallas_call(
        functools.partial(attend_kernel, heads=heads),
        grid=(rows // length,),
        out_shape=jax.ShapeDtypeStruct((rows, value_lanes), BF16),
        in_specs=[
            pl.BlockSpec((length, sums.shape[1]), lambda i: (i, 0)),
            pl.BlockSpec((1, shift.shape[0]), lambda i: (0, 0)),
            pl.BlockSpec((length, shift.shape[0]), lambda i: (i, 0)),
            pl.BlockSpec((1, value_lanes), lambda i: (0, 0)),
        ],
        out_specs=pl.BlockSpec((length, value_lanes), lambda i: (i, 0)),
        compiler_params=pltpu.CompilerParams(vmem_limit_bytes=VMEM_LIMIT),
        name="attend",
    )(sums, shift.reshape(1, -1), spike, scale.astype(F32).reshape(1, -1))


def causal_conv(content_tokens, taps, length):
    rows, columns = content_tokens.shape
    content_tokens = content_tokens.astype(F32).reshape(rows // length, length, columns)
    taps = taps.astype(F32)
    width = taps.shape[0]
    padded = jnp.pad(content_tokens, ((0, 0), (width - 1, 0), (0, 0)))
    total = jnp.zeros_like(content_tokens)
    for offset in range(width):
        total = total + padded[:, offset : offset + length] * taps[offset]
    return total.reshape(rows, columns)


def shards(
    sizes,
    incoming_features,
    attend_prenormal_scale,
    probe_matrix,
    lookup_matrix,
    content_matrix,
    forgetting_matrix,
    result_switch_matrix,
    forgetting_shift,
    spike_forget_logarithm,
    attend_unit_scale,
    attend_result_matrix,
    perceptron_scale,
    content_expand_matrix,
    switch_expand_matrix,
    content_kernel,
    switch_kernel,
    contract_matrix,
):
    n_rep, n_fs, n_tp = sizes
    rep = lax.axis_index("rep")
    length = incoming_features.shape[0]

    def mine(array, axis):
        size = array.shape[axis] // n_rep
        return lax.dynamic_slice_in_dim(array, rep * size, size, axis)

    project = jnp.concatenate(
        [
            mine(matrix, 1)
            for matrix in (
                probe_matrix,
                lookup_matrix,
                content_matrix,
                forgetting_matrix,
                result_switch_matrix,
            )
        ],
        axis=1,
    )
    project_all, whole_in = gather_weights((project,), (0,), incoming_features, sizes, 0)
    spike_all = lax.all_to_all(
        spike_forget_logarithm, "rep", split_axis=1, concat_axis=0, tiled=True
    )
    normed = row_norm(whole_in, attend_prenormal_scale)
    sums = jnp.dot(normed, project_all, preferred_element_type=F32)
    expand = jnp.concatenate([mine(content_expand_matrix, 1), mine(switch_expand_matrix, 1)], axis=1)
    side = attend_result_matrix.shape[1]
    axis = 1 if side % 128 == 0 else 0
    result_all, expand_all, contract_all = gather_weights(
        (mine(attend_result_matrix, 0), expand, mine(contract_matrix, 0)),
        (axis, 0, axis),
        None,
        sizes,
        1,
    )
    if axis == 0:
        result_all, contract_all = (
            array.reshape(n_fs, -1, side).swapaxes(0, 1).reshape(-1, n_fs * side)
            for array in (result_all, contract_all)
        )
    switched_result = attend(
        sums,
        mine(forgetting_shift, 0),
        spike_all,
        mine(attend_unit_scale, 0),
        length,
    )
    mixer_partial = jnp.dot(switched_result, result_all, preferred_element_type=F32).astype(BF16)
    middle, whole_mid = reduce_group(mixer_partial, incoming_features, sizes, True, 2)
    normed_mid = row_norm(whole_mid, perceptron_scale)
    both = jnp.dot(normed_mid, expand_all, preferred_element_type=F32).astype(BF16)
    half = both.shape[1] // 2
    conv_value = causal_conv(both[:, :half], mine(content_kernel, 1), length)
    conv_gated = causal_conv(both[:, half:], mine(switch_kernel, 1), length)
    hidden = (conv_value * jax.nn.gelu(conv_gated, approximate=True)).astype(BF16)
    down_partial = jnp.dot(hidden, contract_all, preferred_element_type=F32).astype(BF16)
    return reduce_group(down_partial, middle, sizes, False, 3)[0]


def solution(mesh):
    sizes = (mesh.shape["rep"], mesh.shape["fs"], mesh.shape["tp"])
    placed = (
        P(("rep", "fs"), "tp"),
        P(),
        P("fs", "tp"),
        P("fs", "tp"),
        P("fs", "tp"),
        P("fs", "tp"),
        P("fs", "tp"),
        P("tp"),
        P(("rep", "fs"), "tp"),
        P("tp"),
        P("tp", "fs"),
        P(),
        P("fs", "tp"),
        P("fs", "tp"),
        P(None, "tp"),
        P(None, "tp"),
        P("tp", "fs"),
    )
    return jax.shard_map(
        functools.partial(shards, sizes),
        mesh=mesh,
        in_specs=placed,
        out_specs=P(("rep", "fs"), "tp"),
        check_vma=False,
    )
```

```python
import functools

import jax
import jax.numpy as jnp
from jax import lax
from jax.experimental import pallas as pl
from jax.experimental.pallas import tpu as pltpu
from jax.sharding import PartitionSpec as P

HEAD_K = 32
HEAD_V = 64
SUB = 16

norm_eps = 1e-06
switch_multiplier = 16.0
MESH = pl.DeviceIdType.MESH
F32 = jnp.float32
BF16 = jnp.bfloat16
HIGHEST = lax.Precision.HIGHEST
VMEM_LIMIT = 60 * 1024 * 1024


def row_norm(content_tokens, gain):
    content_tokens = content_tokens.astype(F32)
    scaled = content_tokens * lax.rsqrt(
        jnp.mean(content_tokens * content_tokens, axis=-1, keepdims=True) + norm_eps
    )
    return (scaled * gain.astype(F32)).astype(BF16)


def factor(n):
    inner = 1
    for size in range(1, n + 1):
        if n % size == 0 and size * size <= n:
            inner = size
    return n // inner, inner


def place(ref, axis, index, size):
    at = pl.ds(pl.multiple_of(index * size, size), size)
    return ref.at[at, :] if axis == 0 else ref.at[:, at]


def send_to(source, target, send_sem, recv_sem, peer):
    copy = pltpu.make_async_remote_copy(
        src_ref=source,
        dst_ref=target,
        send_sem=send_sem,
        recv_sem=recv_sem,
        device_id=peer,
        device_id_type=MESH,
    )
    copy.start()
    return copy


def pieces_of(rows, most):
    for count in range(most, 1, -1):
        if rows % (16 * count) == 0:
            return count
    return 1


def first_half(
    project, result, expand, contract, features, gain, shift, spike, scale, axis, inside, sizes
):
    n_rep, n_fs, n_tp = sizes
    outer, inner = factor(n_fs)
    length, columns = features.shape
    rows = length * n_rep
    heads = shift.shape[0] // HEAD_K
    value_lanes = heads * HEAD_V
    group = n_rep * n_tp
    most = max(n_rep, n_tp)
    weights = (project, result, expand, contract)
    axes = (0, axis, 0, axis)
    splits = (2, 1, 4, 4)
    full = []
    chunks = []
    for w in range(4):
        shape = list(weights[w].shape)
        size = shape[0]
        shape[axes[w]] *= n_fs
        full.append(tuple(shape))
        split = pieces_of(size, splits[w])
        chunks += [(w, k * (size // split), size // split) for k in range(split)]
    count = len(chunks)

    def kernel(*refs):
        sources = refs[:4]
        features_ref, gain_ref, shift_ref, spike_ref, scale_ref = refs[4:9]
        if inside:
            expand_out, contract_out, middle_ref, mid_ref = refs[9:13]
            rest = refs[13:]
            result_out, gated_ref, partial_ref, slot_a, held, slot_b = rest[:6]
            rest = rest[6:]
        else:
            expand_out, contract_out, result_out, gated_ref = refs[9:13]
            rest = refs[13:]
        project_out, whole_ref = rest[:2]
        far_send, far_recv, near_send, near_recv, own_sem, group_send, group_recv = rest[2:9]
        if inside:
            sum_send, sum_recv = rest[9:]
        outs = (project_out, result_out, expand_out, contract_out)
        rep, fs, tp = lax.axis_index("rep"), lax.axis_index("fs"), lax.axis_index("tp")
        a, b = fs // inner, lax.rem(fs, inner)
        far = [lax.rem(a + d, outer) * inner + b for d in range(1, outer)]
        near = [a * inner + lax.rem(b + d, inner) for d in range(1, inner)]
        peers = [{"fs": index} for index in far + near]
        others = [
            {"rep": lax.rem(rep + i, n_rep), "tp": lax.rem(tp + j, n_tp)}
            for i in range(n_rep)
            for j in range(n_tp)
            if i or j
        ]
        barrier = pltpu.get_barrier_semaphore()
        for peer in peers + others:
            pl.semaphore_signal(barrier, inc=1, device_id=peer, device_id_type=MESH)
        pl.semaphore_wait(barrier, len(peers) + len(others))

        def block(w, start, size, index):
            across = weights[w].shape[axes[w]]
            offset = pl.multiple_of(index * across, across)
            if axes[w] == 0:
                return outs[w].at[pl.ds(offset + start, size), :]
            return outs[w].at[pl.ds(start, size), pl.ds(offset, across)]

        far_copies, near_copies, own_copies = {}, {}, {}

        def launch_far(c):
            w, start, size = chunks[c]
            source, target = sources[w].at[pl.ds(start, size), :], block(w, start, size, fs)
            far_copies[c] = [
                send_to(source, target, far_send.at[c, d], far_recv.at[c, d], {"fs": index})
                for d, index in enumerate(far)
            ]

        def launch_near(c):
            w, start, size = chunks[c]
            source, target = sources[w].at[pl.ds(start, size), :], block(w, start, size, fs)
            near_copies[c] = [
                send_to(
                    source, target, near_send.at[c, 0, e], near_recv.at[c, 0, e], {"fs": index}
                )
                for e, index in enumerate(near)
            ]
            own_copies[c] = pltpu.make_async_copy(source, target, own_sem.at[c])
            own_copies[c].start()

        def forward(c):
            w, start, size = chunks[c]
            for d in range(1, outer):
                far_copies[c][d - 1].wait_recv()
                held_block = block(w, start, size, lax.rem(a + outer - d, outer) * inner + b)
                near_copies[c] += [
                    send_to(
                        held_block,
                        held_block,
                        near_send.at[c, d, e],
                        near_recv.at[c, d, e],
                        {"fs": index},
                    )
                    for e, index in enumerate(near)
                ]

        def arrived(c):
            for copy in near_copies[c]:
                copy.wait_recv()
            own_copies[c].wait()

        first = [c for c in range(count) if chunks[c][0] == 0]
        second = [c for c in range(count) if chunks[c][0] == 1]
        later = [c for c in range(count) if chunks[c][0] > 1]

        spot = whole_ref.at[
            pl.ds(pl.multiple_of(rep * length, length), length),
            pl.ds(pl.multiple_of(tp * columns, columns), columns),
        ]
        own = pltpu.make_async_copy(features_ref, spot, own_sem.at[count])
        own.start()
        group_copies = [
            send_to(features_ref, spot, group_send.at[d], group_recv.at[d], peer)
            for d, peer in enumerate(others)
        ]
        for c in first:
            launch_far(c)
            launch_near(c)
        for c in second + later:
            launch_far(c)
        for c in first:
            forward(c)
        for c in second + later:
            launch_near(c)
        for c in first:
            arrived(c)
        own.wait()
        for copy in group_copies:
            copy.wait()

        def sequence(i, carry):
            at = pl.ds(pl.multiple_of(i * length, length), length)
            normed = row_norm(whole_ref[at, :], gain_ref[...])
            sums = jnp.dot(normed, project_out[...], preferred_element_type=F32)
            gated_ref[at, :] = attend_rows(
                sums, shift_ref[...], spike_ref[at, :], scale_ref[...], heads
            )
            return carry

        lax.fori_loop(0, n_rep, sequence, 0)
        for c in second:
            forward(c)
        waiting = list(later)
        for c in waiting[:1]:
            forward(c)
        waiting = waiting[1:]
        for c in second:
            arrived(c)
        if inside:

            def mixer(i, carry):
                at = pl.ds(pl.multiple_of(i * length, length), length)
                partial_ref[at, :] = jnp.dot(
                    gated_ref[at, :], result_out[...], preferred_element_type=F32
                ).astype(BF16)
                return carry

            lax.fori_loop(0, n_rep, mixer, 0)

            def between(stage):
                if stage in (1, 2):
                    forward(waiting.pop(0))

            reduce_steps(
                partial_ref,
                features_ref,
                middle_ref,
                mid_ref,
                slot_a,
                held,
                slot_b,
                sum_send,
                sum_recv,
                sizes,
                between,
            )
        for c in waiting:
            forward(c)
        for c in later:
            arrived(c)
        for c in range(count):
            for copy in far_copies[c] + near_copies[c]:
                copy.wait_send()

    dma = pltpu.SemaphoreType.DMA
    vmem = pl.BlockSpec(memory_space=pltpu.VMEM)
    hbm = pl.BlockSpec(memory_space=pl.ANY)
    out_shape = [jax.ShapeDtypeStruct(full[2], BF16), jax.ShapeDtypeStruct(full[3], BF16)]
    scratch = []
    gated_shape = (rows, value_lanes)
    if inside:
        out_shape += [
            jax.ShapeDtypeStruct((length, columns), BF16),
            jax.ShapeDtypeStruct((rows, columns * n_tp), BF16),
        ]
        out_specs = [hbm, hbm, vmem, vmem]
        scratch += [
            pltpu.VMEM(full[1], BF16),
            pltpu.VMEM(gated_shape, BF16),
            pltpu.VMEM((rows, columns * n_tp), BF16),
            pltpu.VMEM((max(n_tp - 1, 1), rows, columns), BF16),
            pltpu.VMEM((rows, columns), BF16),
            pltpu.VMEM((max(n_rep - 1, 1), length, columns), BF16),
        ]
    else:
        out_shape += [
            jax.ShapeDtypeStruct(full[1], BF16),
            jax.ShapeDtypeStruct(gated_shape, BF16),
        ]
        out_specs = [hbm, hbm, hbm, vmem]
    scratch += [
        pltpu.VMEM(full[0], BF16),
        pltpu.VMEM((rows, columns * n_tp), BF16),
        dma((count, max(outer - 1, 1))),
        dma((count, max(outer - 1, 1))),
        dma((count, outer, max(inner - 1, 1))),
        dma((count, outer, max(inner - 1, 1))),
        dma((count + 1,)),
        dma((group,)),
        dma((group,)),
    ]
    if inside:
        scratch += [dma((4, most)), dma((4, most))]
    return pl.pallas_call(
        kernel,
        out_shape=out_shape,
        in_specs=[vmem] * 9,
        out_specs=out_specs,
        scratch_shapes=scratch,
        compiler_params=pltpu.CompilerParams(
            collective_id=0, has_side_effects=True, vmem_limit_bytes=VMEM_LIMIT
        ),
        name="first_half",
    )(
        *weights,
        features,
        gain.reshape(1, -1),
        shift.reshape(1, -1),
        spike,
        scale.astype(F32).reshape(1, -1),
    )


def reduce_steps(
    part_ref, base_ref, out_ref, all_ref, slot_a, held, slot_b, send_sem, recv_sem, sizes, between
):
    n_rep, n_fs, n_tp = sizes
    rows, columns = base_ref.shape
    rep, tp = lax.axis_index("rep"), lax.axis_index("tp")
    tps = [lax.rem(tp + d, n_tp) for d in range(1, n_tp)]
    reps = [lax.rem(rep + d, n_rep) for d in range(1, n_rep)]

    def send(stage, d, source, target, peer):
        return send_to(source, target, send_sem.at[stage, d], recv_sem.at[stage, d], peer)

    copies = [
        send(0, d, place(part_ref, 1, index, columns), slot_a.at[d], {"tp": index})
        for d, index in enumerate(tps)
    ]
    for copy in copies:
        copy.wait()
    total = place(part_ref, 1, tp, columns)[...].astype(F32)
    for d in range(len(tps)):
        total = total + slot_a[d].astype(F32)
    held[...] = total.astype(BF16)
    copies = [
        send(1, d, place(held, 0, index, rows), slot_b.at[d], {"rep": index})
        for d, index in enumerate(reps)
    ]
    between(1)
    for copy in copies:
        copy.wait()
    total = place(held, 0, rep, rows)[...].astype(F32)
    for d in range(len(reps)):
        total = total + slot_b[d].astype(F32)
    result = (base_ref[...].astype(F32) + total.astype(BF16).astype(F32)).astype(BF16)
    out_ref[...] = result
    if all_ref is not None:
        block = all_ref.at[
            pl.ds(pl.multiple_of(rep * rows, rows), rows),
            pl.ds(pl.multiple_of(tp * columns, columns), columns),
        ]
        block[...] = result
        copies = [send(2, d, block, block, {"rep": index}) for d, index in enumerate(reps)]
        between(2)
        for copy in copies:
            copy.wait()
        strip = place(all_ref, 1, tp, columns)
        copies = [send(3, d, strip, strip, {"tp": index}) for d, index in enumerate(tps)]
        for copy in copies:
            copy.wait()


def reduce_group(partial, base, sizes, spread, collective_id):
    n_rep, n_fs, n_tp = sizes
    rows, columns = base.shape

    def kernel(*refs):
        part_ref, base_ref = refs[:2]
        if spread:
            out_ref, all_ref, slot_a, held, slot_b, send_sem, recv_sem = refs[2:]
        else:
            all_ref = None
            out_ref, slot_a, held, slot_b, send_sem, recv_sem = refs[2:]
        rep, tp = lax.axis_index("rep"), lax.axis_index("tp")
        barrier = pltpu.get_barrier_semaphore()
        for d in range(1, n_tp):
            peer = {"tp": lax.rem(tp + d, n_tp)}
            pl.semaphore_signal(barrier, inc=1, device_id=peer, device_id_type=MESH)
        for d in range(1, n_rep):
            peer = {"rep": lax.rem(rep + d, n_rep)}
            pl.semaphore_signal(barrier, inc=1, device_id=peer, device_id_type=MESH)
        pl.semaphore_wait(barrier, n_tp + n_rep - 2)
        reduce_steps(
            part_ref,
            base_ref,
            out_ref,
            all_ref,
            slot_a,
            held,
            slot_b,
            send_sem,
            recv_sem,
            sizes,
            lambda stage: None,
        )

    out_shape = [jax.ShapeDtypeStruct((rows, columns), BF16)]
    if spread:
        out_shape.append(jax.ShapeDtypeStruct((rows * n_rep, columns * n_tp), BF16))
    vmem = pl.BlockSpec(memory_space=pltpu.VMEM)
    most = max(n_rep, n_tp)
    return pl.pallas_call(
        kernel,
        out_shape=out_shape,
        in_specs=[vmem, vmem],
        out_specs=[vmem] * len(out_shape),
        scratch_shapes=[
            pltpu.VMEM((max(n_tp - 1, 1), rows * n_rep, columns), BF16),
            pltpu.VMEM((rows * n_rep, columns), BF16),
            pltpu.VMEM((max(n_rep - 1, 1), rows, columns), BF16),
            pltpu.SemaphoreType.DMA((4, most)),
            pltpu.SemaphoreType.DMA((4, most)),
        ],
        compiler_params=pltpu.CompilerParams(
            collective_id=collective_id, has_side_effects=True, vmem_limit_bytes=VMEM_LIMIT
        ),
        name="reduce_group",
    )(partial, base)


def lanes_same(shape, row_width, column_width):
    return (
        lax.broadcasted_iota(jnp.int32, shape, 0) // row_width
        == lax.broadcasted_iota(jnp.int32, shape, 1) // column_width
    ).astype(F32)


def dot32(left, right, contract=((1,), (0,))):
    return lax.dot_general(
        left, right, (contract, ((), ())), precision=HIGHEST, preferred_element_type=F32
    )


def attend_rows(sums, shift, spike, scale, heads):
    length = sums.shape[0]
    key_lanes, value_lanes = heads * HEAD_K, heads * HEAD_V

    def part(start, width):
        return sums[:, start : start + width]

    def rounded(array):
        return array.astype(BF16).astype(F32)

    query = rounded(part(0, key_lanes)) * HEAD_K ** (-0.5)
    keys = rounded(part(key_lanes, key_lanes))
    values = rounded(part(2 * key_lanes, value_lanes))
    decay_pre = part(2 * key_lanes + value_lanes, key_lanes) + shift
    gate = rounded(part(3 * key_lanes + value_lanes, value_lanes))
    log_sigmoid = jnp.minimum(decay_pre, 0.0) - jnp.log1p(jnp.exp(-jnp.abs(decay_pre)))
    c = log_sigmoid / switch_multiplier + spike
    row = lax.broadcasted_iota(jnp.int32, (length, key_lanes), 0)
    step = 1
    while step < length:
        c = c + jnp.where(row >= step, pltpu.roll(c, step, 0), 0.0)
        step *= 2

    spread = lanes_same((key_lanes, value_lanes), HEAD_K, HEAD_V)
    in_sub = lax.rem(row, SUB)
    out = dot32(query * keys, spread) * values
    for d in range(1, SUB):
        ok = in_sub >= d
        weight = jnp.exp(jnp.where(ok, c - pltpu.roll(c, d, 0), 0.0))
        product = jnp.where(ok, query * pltpu.roll(keys, d, 0) * weight, 0.0)
        out = out + dot32(product, spread) * pltpu.roll(values, d, 0)

    pieces = [jnp.zeros((SUB, value_lanes), F32)]
    stack = heads * SUB
    key_mask = lanes_same((stack, key_lanes), SUB, HEAD_K)
    value_mask = lanes_same((stack, value_lanes), SUB, HEAD_V)
    for start in range(SUB, length, SUB):
        edge = c[start - 1 : start]
        q_part = query[start : start + SUB] * jnp.exp(c[start : start + SUB] - edge)
        k_part = keys[:start] * jnp.exp(edge - c[:start])
        stacked = jnp.concatenate([q_part] * heads, axis=0) * key_mask
        scores = dot32(stacked, k_part, ((1,), (1,)))
        read = dot32(scores, values[:start]) * value_mask
        total = read[:SUB]
        for h in range(1, heads):
            total = total + read[h * SUB : (h + 1) * SUB]
        pieces.append(total)
    out = out + jnp.concatenate(pieces, axis=0)

    same = lanes_same((value_lanes, value_lanes), HEAD_V, HEAD_V)
    mean = dot32(out * out, same) / HEAD_V
    out = out * lax.rsqrt(mean + norm_eps) * scale
    return (out * (gate / (1.0 + jnp.exp(-gate)))).astype(BF16)


def causal_conv(content_tokens, taps, length):
    rows, columns = content_tokens.shape
    content_tokens = content_tokens.astype(F32).reshape(rows // length, length, columns)
    taps = taps.astype(F32)
    width = taps.shape[0]
    padded = jnp.pad(content_tokens, ((0, 0), (width - 1, 0), (0, 0)))
    total = jnp.zeros_like(content_tokens)
    for offset in range(width):
        total = total + padded[:, offset : offset + length] * taps[offset]
    return total.reshape(rows, columns)


def shards(
    sizes,
    incoming_features,
    attend_prenormal_scale,
    probe_matrix,
    lookup_matrix,
    content_matrix,
    forgetting_matrix,
    result_switch_matrix,
    forgetting_shift,
    spike_forget_logarithm,
    attend_unit_scale,
    attend_result_matrix,
    perceptron_scale,
    content_expand_matrix,
    switch_expand_matrix,
    content_kernel,
    switch_kernel,
    contract_matrix,
):
    n_rep, n_fs, n_tp = sizes
    rep = lax.axis_index("rep")
    length = incoming_features.shape[0]

    def mine(array, axis):
        size = array.shape[axis] // n_rep
        return lax.dynamic_slice_in_dim(array, rep * size, size, axis)

    project = jnp.concatenate(
        [
            mine(matrix, 1)
            for matrix in (
                probe_matrix,
                lookup_matrix,
                content_matrix,
                forgetting_matrix,
                result_switch_matrix,
            )
        ],
        axis=1,
    )
    spike_all = lax.all_to_all(
        spike_forget_logarithm, "rep", split_axis=1, concat_axis=0, tiled=True
    )
    expand = jnp.concatenate([mine(content_expand_matrix, 1), mine(switch_expand_matrix, 1)], axis=1)
    side = attend_result_matrix.shape[1]
    inside = side % 128 == 0
    outs = first_half(
        project,
        mine(attend_result_matrix, 0),
        expand,
        mine(contract_matrix, 0),
        incoming_features,
        attend_prenormal_scale,
        mine(forgetting_shift, 0),
        spike_all,
        mine(attend_unit_scale, 0),
        1 if inside else 0,
        inside,
        sizes,
    )
    if inside:
        expand_all, contract_all, middle, whole_mid = outs
    else:
        expand_all, contract_all, result_all, switched_result = outs
        result_all, contract_all = (
            array.reshape(n_fs, -1, side).swapaxes(0, 1).reshape(-1, n_fs * side)
            for array in (result_all, contract_all)
        )
        mixer_partial = jnp.dot(switched_result, result_all, preferred_element_type=F32)
        middle, whole_mid = reduce_group(
            mixer_partial.astype(BF16), incoming_features, sizes, True, 2
        )
    normed_mid = row_norm(whole_mid, perceptron_scale)
    both = jnp.dot(normed_mid, expand_all, preferred_element_type=F32).astype(BF16)
    half = both.shape[1] // 2
    conv_value = causal_conv(both[:, :half], mine(content_kernel, 1), length)
    conv_gated = causal_conv(both[:, half:], mine(switch_kernel, 1), length)
    hidden = (conv_value * jax.nn.gelu(conv_gated, approximate=True)).astype(BF16)
    down_partial = jnp.dot(hidden, contract_all, preferred_element_type=F32).astype(BF16)
    return reduce_group(down_partial, middle, sizes, False, 3)[0]


def solution(mesh):
    sizes = (mesh.shape["rep"], mesh.shape["fs"], mesh.shape["tp"])
    placed = (
        P(("rep", "fs"), "tp"),
        P(),
        P("fs", "tp"),
        P("fs", "tp"),
        P("fs", "tp"),
        P("fs", "tp"),
        P("fs", "tp"),
        P("tp"),
        P(("rep", "fs"), "tp"),
        P("tp"),
        P("tp", "fs"),
        P(),
        P("fs", "tp"),
        P("fs", "tp"),
        P(None, "tp"),
        P(None, "tp"),
        P("tp", "fs"),
    )
    return jax.shard_map(
        functools.partial(shards, sizes),
        mesh=mesh,
        in_specs=placed,
        out_specs=P(("rep", "fs"), "tp"),
        check_vma=False,
    )
```

```python
import functools

import jax
import jax.numpy as jnp
from jax import lax
from jax.experimental import pallas as pl
from jax.experimental.pallas import tpu as pltpu
from jax.sharding import PartitionSpec as P

HEAD_K = 32
HEAD_V = 64
SUB = 16

norm_eps = 1e-06
switch_multiplier = 16.0
MESH = pl.DeviceIdType.MESH
F32 = jnp.float32
BF16 = jnp.bfloat16
HIGHEST = lax.Precision.HIGHEST
VMEM_LIMIT = 60 * 1024 * 1024


def row_norm(content_tokens, gain):
    content_tokens = content_tokens.astype(F32)
    scaled = content_tokens * lax.rsqrt(
        jnp.mean(content_tokens * content_tokens, axis=-1, keepdims=True) + norm_eps
    )
    return (scaled * gain.astype(F32)).astype(BF16)


def factor(n):
    inner = 1
    for size in range(1, n + 1):
        if n % size == 0 and size * size <= n:
            inner = size
    return n // inner, inner


def place(ref, axis, index, size):
    at = pl.ds(pl.multiple_of(index * size, size), size)
    return ref.at[at, :] if axis == 0 else ref.at[:, at]


def send_to(source, target, send_sem, recv_sem, peer):
    copy = pltpu.make_async_remote_copy(
        src_ref=source,
        dst_ref=target,
        send_sem=send_sem,
        recv_sem=recv_sem,
        device_id=peer,
        device_id_type=MESH,
    )
    copy.start()
    return copy


def pieces_of(rows, most):
    for count in range(most, 1, -1):
        if rows % (16 * count) == 0:
            return count
    return 1


def first_half(
    project, result, expand, contract, features, gain, shift, spike, scale, axis, inside, sizes
):
    n_rep, n_fs, n_tp = sizes
    outer, inner = factor(n_fs)
    length, columns = features.shape
    rows = length * n_rep
    heads = shift.shape[0] // HEAD_K
    value_lanes = heads * HEAD_V
    group = n_rep * n_tp
    most = max(n_rep, n_tp)
    weights = (project, result, expand, contract)
    axes = (0, axis, 0, axis)
    splits = (2, 1, 4, 4)
    full = []
    chunks = []
    for w in range(4):
        shape = list(weights[w].shape)
        size = shape[0]
        shape[axes[w]] *= n_fs
        full.append(tuple(shape))
        split = pieces_of(size, splits[w])
        chunks += [(w, k * (size // split), size // split) for k in range(split)]
    count = len(chunks)

    def kernel(*refs):
        sources = refs[:4]
        features_ref, gain_ref, shift_ref, spike_ref, scale_ref = refs[4:9]
        if inside:
            expand_out, contract_out, middle_ref, mid_ref = refs[9:13]
            rest = refs[13:]
            result_out, gated_ref, partial_ref, slot_a, held, slot_b = rest[:6]
            rest = rest[6:]
        else:
            expand_out, contract_out, result_out, gated_ref = refs[9:13]
            rest = refs[13:]
        project_out, whole_ref = rest[:2]
        far_send, far_recv, near_send, near_recv, own_sem, group_send, group_recv = rest[2:9]
        if inside:
            sum_send, sum_recv = rest[9:]
        outs = (project_out, result_out, expand_out, contract_out)
        rep, fs, tp = lax.axis_index("rep"), lax.axis_index("fs"), lax.axis_index("tp")
        a, b = fs // inner, lax.rem(fs, inner)
        far = [lax.rem(a + d, outer) * inner + b for d in range(1, outer)]
        near = [a * inner + lax.rem(b + d, inner) for d in range(1, inner)]
        peers = [{"fs": index} for index in far + near]
        others = [
            {"rep": lax.rem(rep + i, n_rep), "tp": lax.rem(tp + j, n_tp)}
            for i in range(n_rep)
            for j in range(n_tp)
            if i or j
        ]
        barrier = pltpu.get_barrier_semaphore()
        for peer in peers + others:
            pl.semaphore_signal(barrier, inc=1, device_id=peer, device_id_type=MESH)
        pl.semaphore_wait(barrier, len(peers) + len(others))

        def block(w, start, size, index):
            across = weights[w].shape[axes[w]]
            offset = pl.multiple_of(index * across, across)
            if axes[w] == 0:
                return outs[w].at[pl.ds(offset + start, size), :]
            return outs[w].at[pl.ds(start, size), pl.ds(offset, across)]

        near_copies, own_copies = {}, {}

        def hop(c, step, way):
            w, start, size = chunks[c]
            spot = block(w, start, size, (a - way * step) * inner + b)
            source = sources[w].at[pl.ds(start, size), :] if step == 0 else spot
            at = step if way > 0 else outer - 1 + step
            return pltpu.make_async_remote_copy(
                src_ref=source,
                dst_ref=spot,
                send_sem=far_send.at[c, at],
                recv_sem=far_recv.at[c, at],
                device_id={"fs": (a + way) * inner + b},
                device_id_type=MESH,
            )

        def turn(c, step, way, e):
            w, start, size = chunks[c]
            spot = block(w, start, size, (a - way * step) * inner + b)
            at = step if way > 0 else outer - 1 + step
            return pltpu.make_async_remote_copy(
                src_ref=spot,
                dst_ref=spot,
                send_sem=near_send.at[c, at, e],
                recv_sem=near_recv.at[c, at, e],
                device_id={"fs": near[e]},
                device_id_type=MESH,
            )

        def has(step, way):
            return a >= step if way > 0 else a + step < outer

        def goes(way):
            return a + 1 < outer if way > 0 else a >= 1

        def launch_far(c):
            for way in (1, -1):

                @pl.when(goes(way))
                def _(way=way):
                    hop(c, 0, way).start()

        def forward(c):
            for step in range(1, outer):
                for way in (1, -1):

                    @pl.when(has(step, way))
                    def _(step=step, way=way):
                        hop_in = hop(c, step - 1, way)
                        hop_in.wait_recv()
                        if step + 1 < outer:

                            @pl.when(goes(way))
                            def _():
                                hop(c, step, way).start()

                        for e in range(len(near)):
                            turn(c, step, way, e).start()

        def sent(c):
            for way in (1, -1):

                @pl.when(goes(way))
                def _(way=way):
                    hop(c, 0, way).wait_send()

            for step in range(1, outer):
                for way in (1, -1):

                    @pl.when(has(step, way))
                    def _(step=step, way=way):
                        if step + 1 < outer:

                            @pl.when(goes(way))
                            def _():
                                hop(c, step, way).wait_send()

                        for e in range(len(near)):
                            turn(c, step, way, e).wait_send()

        def launch_near(c):
            w, start, size = chunks[c]
            source, target = sources[w].at[pl.ds(start, size), :], block(w, start, size, fs)
            near_copies[c] = [
                send_to(
                    source, target, near_send.at[c, 0, e], near_recv.at[c, 0, e], {"fs": index}
                )
                for e, index in enumerate(near)
            ]
            own_copies[c] = pltpu.make_async_copy(source, target, own_sem.at[c])
            own_copies[c].start()

        def arrived(c):
            for copy in near_copies[c]:
                copy.wait_recv()
            own_copies[c].wait()
            for step in range(1, outer):
                for way in (1, -1):

                    @pl.when(has(step, way))
                    def _(step=step, way=way):
                        for e in range(len(near)):
                            turn(c, step, way, e).wait_recv()


        first = [c for c in range(count) if chunks[c][0] == 0]
        second = [c for c in range(count) if chunks[c][0] == 1]
        later = [c for c in range(count) if chunks[c][0] > 1]

        spot = whole_ref.at[
            pl.ds(pl.multiple_of(rep * length, length), length),
            pl.ds(pl.multiple_of(tp * columns, columns), columns),
        ]
        own = pltpu.make_async_copy(features_ref, spot, own_sem.at[count])
        own.start()
        group_copies = [
            send_to(features_ref, spot, group_send.at[d], group_recv.at[d], peer)
            for d, peer in enumerate(others)
        ]
        for c in first:
            launch_far(c)
            launch_near(c)
        for c in second + later:
            launch_far(c)
        for c in first:
            forward(c)
        for c in second + later:
            launch_near(c)
        for c in first:
            arrived(c)
        own.wait()
        for copy in group_copies:
            copy.wait()

        def sequence(i, carry):
            at = pl.ds(pl.multiple_of(i * length, length), length)
            normed = row_norm(whole_ref[at, :], gain_ref[...])
            sums = jnp.dot(normed, project_out[...], preferred_element_type=F32)
            gated_ref[at, :] = attend_rows(
                sums, shift_ref[...], spike_ref[at, :], scale_ref[...], heads
            )
            return carry

        lax.fori_loop(0, n_rep, sequence, 0)
        for c in second:
            forward(c)
        waiting = list(later)
        for c in waiting[:1]:
            forward(c)
        waiting = waiting[1:]
        for c in second:
            arrived(c)
        if inside:

            def mixer(i, carry):
                at = pl.ds(pl.multiple_of(i * length, length), length)
                partial_ref[at, :] = jnp.dot(
                    gated_ref[at, :], result_out[...], preferred_element_type=F32
                ).astype(BF16)
                return carry

            lax.fori_loop(0, n_rep, mixer, 0)

            def between(stage):
                if stage in (1, 2):
                    forward(waiting.pop(0))

            reduce_steps(
                partial_ref,
                features_ref,
                middle_ref,
                mid_ref,
                slot_a,
                held,
                slot_b,
                sum_send,
                sum_recv,
                sizes,
                between,
            )
        for c in waiting:
            forward(c)
        for c in later:
            arrived(c)
        for c in range(count):
            for copy in near_copies[c]:
                copy.wait_send()
            sent(c)

    dma = pltpu.SemaphoreType.DMA
    vmem = pl.BlockSpec(memory_space=pltpu.VMEM)
    hbm = pl.BlockSpec(memory_space=pl.ANY)
    out_shape = [jax.ShapeDtypeStruct(full[2], BF16), jax.ShapeDtypeStruct(full[3], BF16)]
    scratch = []
    gated_shape = (rows, value_lanes)
    if inside:
        out_shape += [
            jax.ShapeDtypeStruct((length, columns), BF16),
            jax.ShapeDtypeStruct((rows, columns * n_tp), BF16),
        ]
        out_specs = [hbm, hbm, vmem, vmem]
        scratch += [
            pltpu.VMEM(full[1], BF16),
            pltpu.VMEM(gated_shape, BF16),
            pltpu.VMEM((rows, columns * n_tp), BF16),
            pltpu.VMEM((max(n_tp - 1, 1), rows, columns), BF16),
            pltpu.VMEM((rows, columns), BF16),
            pltpu.VMEM((max(n_rep - 1, 1), length, columns), BF16),
        ]
    else:
        out_shape += [
            jax.ShapeDtypeStruct(full[1], BF16),
            jax.ShapeDtypeStruct(gated_shape, BF16),
        ]
        out_specs = [hbm, hbm, hbm, vmem]
    scratch += [
        pltpu.VMEM(full[0], BF16),
        pltpu.VMEM((rows, columns * n_tp), BF16),
        dma((count, 2 * outer)),
        dma((count, 2 * outer)),
        dma((count, 2 * outer, max(inner - 1, 1))),
        dma((count, 2 * outer, max(inner - 1, 1))),
        dma((count + 1,)),
        dma((group,)),
        dma((group,)),
    ]
    if inside:
        scratch += [dma((4, most)), dma((4, most))]
    return pl.pallas_call(
        kernel,
        out_shape=out_shape,
        in_specs=[vmem] * 9,
        out_specs=out_specs,
        scratch_shapes=scratch,
        compiler_params=pltpu.CompilerParams(
            collective_id=0, has_side_effects=True, vmem_limit_bytes=VMEM_LIMIT
        ),
        name="first_half",
    )(
        *weights,
        features,
        gain.reshape(1, -1),
        shift.reshape(1, -1),
        spike,
        scale.astype(F32).reshape(1, -1),
    )


def reduce_steps(
    part_ref, base_ref, out_ref, all_ref, slot_a, held, slot_b, send_sem, recv_sem, sizes, between
):
    n_rep, n_fs, n_tp = sizes
    rows, columns = base_ref.shape
    rep, tp = lax.axis_index("rep"), lax.axis_index("tp")
    tps = [lax.rem(tp + d, n_tp) for d in range(1, n_tp)]
    reps = [lax.rem(rep + d, n_rep) for d in range(1, n_rep)]

    def send(stage, d, source, target, peer):
        return send_to(source, target, send_sem.at[stage, d], recv_sem.at[stage, d], peer)

    copies = [
        send(0, d, place(part_ref, 1, index, columns), slot_a.at[d], {"tp": index})
        for d, index in enumerate(tps)
    ]
    for copy in copies:
        copy.wait()
    total = place(part_ref, 1, tp, columns)[...].astype(F32)
    for d in range(len(tps)):
        total = total + slot_a[d].astype(F32)
    held[...] = total.astype(BF16)
    copies = [
        send(1, d, place(held, 0, index, rows), slot_b.at[d], {"rep": index})
        for d, index in enumerate(reps)
    ]
    between(1)
    for copy in copies:
        copy.wait()
    total = place(held, 0, rep, rows)[...].astype(F32)
    for d in range(len(reps)):
        total = total + slot_b[d].astype(F32)
    result = (base_ref[...].astype(F32) + total.astype(BF16).astype(F32)).astype(BF16)
    out_ref[...] = result
    if all_ref is not None:
        block = all_ref.at[
            pl.ds(pl.multiple_of(rep * rows, rows), rows),
            pl.ds(pl.multiple_of(tp * columns, columns), columns),
        ]
        block[...] = result
        copies = [send(2, d, block, block, {"rep": index}) for d, index in enumerate(reps)]
        between(2)
        for copy in copies:
            copy.wait()
        strip = place(all_ref, 1, tp, columns)
        copies = [send(3, d, strip, strip, {"tp": index}) for d, index in enumerate(tps)]
        for copy in copies:
            copy.wait()


def reduce_group(partial, base, sizes, spread, collective_id):
    n_rep, n_fs, n_tp = sizes
    rows, columns = base.shape

    def kernel(*refs):
        part_ref, base_ref = refs[:2]
        if spread:
            out_ref, all_ref, slot_a, held, slot_b, send_sem, recv_sem = refs[2:]
        else:
            all_ref = None
            out_ref, slot_a, held, slot_b, send_sem, recv_sem = refs[2:]
        rep, tp = lax.axis_index("rep"), lax.axis_index("tp")
        barrier = pltpu.get_barrier_semaphore()
        for d in range(1, n_tp):
            peer = {"tp": lax.rem(tp + d, n_tp)}
            pl.semaphore_signal(barrier, inc=1, device_id=peer, device_id_type=MESH)
        for d in range(1, n_rep):
            peer = {"rep": lax.rem(rep + d, n_rep)}
            pl.semaphore_signal(barrier, inc=1, device_id=peer, device_id_type=MESH)
        pl.semaphore_wait(barrier, n_tp + n_rep - 2)
        reduce_steps(
            part_ref,
            base_ref,
            out_ref,
            all_ref,
            slot_a,
            held,
            slot_b,
            send_sem,
            recv_sem,
            sizes,
            lambda stage: None,
        )

    out_shape = [jax.ShapeDtypeStruct((rows, columns), BF16)]
    if spread:
        out_shape.append(jax.ShapeDtypeStruct((rows * n_rep, columns * n_tp), BF16))
    vmem = pl.BlockSpec(memory_space=pltpu.VMEM)
    most = max(n_rep, n_tp)
    return pl.pallas_call(
        kernel,
        out_shape=out_shape,
        in_specs=[vmem, vmem],
        out_specs=[vmem] * len(out_shape),
        scratch_shapes=[
            pltpu.VMEM((max(n_tp - 1, 1), rows * n_rep, columns), BF16),
            pltpu.VMEM((rows * n_rep, columns), BF16),
            pltpu.VMEM((max(n_rep - 1, 1), rows, columns), BF16),
            pltpu.SemaphoreType.DMA((4, most)),
            pltpu.SemaphoreType.DMA((4, most)),
        ],
        compiler_params=pltpu.CompilerParams(
            collective_id=collective_id, has_side_effects=True, vmem_limit_bytes=VMEM_LIMIT
        ),
        name="reduce_group",
    )(partial, base)


def lanes_same(shape, row_width, column_width):
    return (
        lax.broadcasted_iota(jnp.int32, shape, 0) // row_width
        == lax.broadcasted_iota(jnp.int32, shape, 1) // column_width
    ).astype(F32)


def dot32(left, right, contract=((1,), (0,))):
    return lax.dot_general(
        left, right, (contract, ((), ())), precision=HIGHEST, preferred_element_type=F32
    )


def attend_rows(sums, shift, spike, scale, heads):
    length = sums.shape[0]
    key_lanes, value_lanes = heads * HEAD_K, heads * HEAD_V

    def part(start, width):
        return sums[:, start : start + width]

    def rounded(array):
        return array.astype(BF16).astype(F32)

    query = rounded(part(0, key_lanes)) * HEAD_K ** (-0.5)
    keys = rounded(part(key_lanes, key_lanes))
    values = rounded(part(2 * key_lanes, value_lanes))
    decay_pre = part(2 * key_lanes + value_lanes, key_lanes) + shift
    gate = rounded(part(3 * key_lanes + value_lanes, value_lanes))
    log_sigmoid = jnp.minimum(decay_pre, 0.0) - jnp.log1p(jnp.exp(-jnp.abs(decay_pre)))
    c = log_sigmoid / switch_multiplier + spike
    row = lax.broadcasted_iota(jnp.int32, (length, key_lanes), 0)
    step = 1
    while step < length:
        c = c + jnp.where(row >= step, pltpu.roll(c, step, 0), 0.0)
        step *= 2

    spread = lanes_same((key_lanes, value_lanes), HEAD_K, HEAD_V)
    in_sub = lax.rem(row, SUB)
    out = dot32(query * keys, spread) * values
    for d in range(1, SUB):
        ok = in_sub >= d
        weight = jnp.exp(jnp.where(ok, c - pltpu.roll(c, d, 0), 0.0))
        product = jnp.where(ok, query * pltpu.roll(keys, d, 0) * weight, 0.0)
        out = out + dot32(product, spread) * pltpu.roll(values, d, 0)

    pieces = [jnp.zeros((SUB, value_lanes), F32)]
    stack = heads * SUB
    key_mask = lanes_same((stack, key_lanes), SUB, HEAD_K)
    value_mask = lanes_same((stack, value_lanes), SUB, HEAD_V)
    for start in range(SUB, length, SUB):
        edge = c[start - 1 : start]
        q_part = query[start : start + SUB] * jnp.exp(c[start : start + SUB] - edge)
        k_part = keys[:start] * jnp.exp(edge - c[:start])
        stacked = jnp.concatenate([q_part] * heads, axis=0) * key_mask
        scores = dot32(stacked, k_part, ((1,), (1,)))
        read = dot32(scores, values[:start]) * value_mask
        total = read[:SUB]
        for h in range(1, heads):
            total = total + read[h * SUB : (h + 1) * SUB]
        pieces.append(total)
    out = out + jnp.concatenate(pieces, axis=0)

    same = lanes_same((value_lanes, value_lanes), HEAD_V, HEAD_V)
    mean = dot32(out * out, same) / HEAD_V
    out = out * lax.rsqrt(mean + norm_eps) * scale
    return (out * (gate / (1.0 + jnp.exp(-gate)))).astype(BF16)


def causal_conv(content_tokens, taps, length):
    rows, columns = content_tokens.shape
    content_tokens = content_tokens.astype(F32).reshape(rows // length, length, columns)
    taps = taps.astype(F32)
    width = taps.shape[0]
    padded = jnp.pad(content_tokens, ((0, 0), (width - 1, 0), (0, 0)))
    total = jnp.zeros_like(content_tokens)
    for offset in range(width):
        total = total + padded[:, offset : offset + length] * taps[offset]
    return total.reshape(rows, columns)


def shards(
    sizes,
    incoming_features,
    attend_prenormal_scale,
    probe_matrix,
    lookup_matrix,
    content_matrix,
    forgetting_matrix,
    result_switch_matrix,
    forgetting_shift,
    spike_forget_logarithm,
    attend_unit_scale,
    attend_result_matrix,
    perceptron_scale,
    content_expand_matrix,
    switch_expand_matrix,
    content_kernel,
    switch_kernel,
    contract_matrix,
):
    n_rep, n_fs, n_tp = sizes
    rep = lax.axis_index("rep")
    length = incoming_features.shape[0]

    def mine(array, axis):
        size = array.shape[axis] // n_rep
        return lax.dynamic_slice_in_dim(array, rep * size, size, axis)

    project = jnp.concatenate(
        [
            mine(matrix, 1)
            for matrix in (
                probe_matrix,
                lookup_matrix,
                content_matrix,
                forgetting_matrix,
                result_switch_matrix,
            )
        ],
        axis=1,
    )
    spike_all = lax.all_to_all(
        spike_forget_logarithm, "rep", split_axis=1, concat_axis=0, tiled=True
    )
    expand = jnp.concatenate([mine(content_expand_matrix, 1), mine(switch_expand_matrix, 1)], axis=1)
    side = attend_result_matrix.shape[1]
    inside = side % 128 == 0
    outs = first_half(
        project,
        mine(attend_result_matrix, 0),
        expand,
        mine(contract_matrix, 0),
        incoming_features,
        attend_prenormal_scale,
        mine(forgetting_shift, 0),
        spike_all,
        mine(attend_unit_scale, 0),
        1 if inside else 0,
        inside,
        sizes,
    )
    if inside:
        expand_all, contract_all, middle, whole_mid = outs
    else:
        expand_all, contract_all, result_all, switched_result = outs
        result_all, contract_all = (
            array.reshape(n_fs, -1, side).swapaxes(0, 1).reshape(-1, n_fs * side)
            for array in (result_all, contract_all)
        )
        mixer_partial = jnp.dot(switched_result, result_all, preferred_element_type=F32)
        middle, whole_mid = reduce_group(
            mixer_partial.astype(BF16), incoming_features, sizes, True, 2
        )
    normed_mid = row_norm(whole_mid, perceptron_scale)
    both = jnp.dot(normed_mid, expand_all, preferred_element_type=F32).astype(BF16)
    half = both.shape[1] // 2
    conv_value = causal_conv(both[:, :half], mine(content_kernel, 1), length)
    conv_gated = causal_conv(both[:, half:], mine(switch_kernel, 1), length)
    hidden = (conv_value * jax.nn.gelu(conv_gated, approximate=True)).astype(BF16)
    down_partial = jnp.dot(hidden, contract_all, preferred_element_type=F32).astype(BF16)
    return reduce_group(down_partial, middle, sizes, False, 3)[0]


def solution(mesh):
    sizes = (mesh.shape["rep"], mesh.shape["fs"], mesh.shape["tp"])
    placed = (
        P(("rep", "fs"), "tp"),
        P(),
        P("fs", "tp"),
        P("fs", "tp"),
        P("fs", "tp"),
        P("fs", "tp"),
        P("fs", "tp"),
        P("tp"),
        P(("rep", "fs"), "tp"),
        P("tp"),
        P("tp", "fs"),
        P(),
        P("fs", "tp"),
        P("fs", "tp"),
        P(None, "tp"),
        P(None, "tp"),
        P("tp", "fs"),
    )
    return jax.shard_map(
        functools.partial(shards, sizes),
        mesh=mesh,
        in_specs=placed,
        out_specs=P(("rep", "fs"), "tp"),
        check_vma=False,
    )
```
